32 devices in a mesh: grp: 2 (over x), ep: 16 (over z, y, core).
Axes of the slice: x: 2, y: 2, z: 4, core: 2. Of those that a mesh axis runs over, the one named last changes fastest.
Arguments:
- sequence_input_rows: bfloat16 [224, 2048], P(('grp', 'ep')), parts along dimension 0, may hold values from -6 to 6
- value_key_state: float32 [224, 32, 64, 64], P(('grp', 'ep')), parts along dimension 0, may hold values from -4 to 4
- receptance_matrix: bfloat16 [2048, 2048], P(None, 'ep'), may hold values from -0.125 to 0.125
- key_matrix: bfloat16 [2048, 2048], P(None, 'ep'), may hold values from -0.125 to 0.125
- value_matrix: bfloat16 [2048, 2048], P(None, 'ep'), may hold values from -0.125 to 0.125
- decay_lowrank_input: bfloat16 [2048, 64], replicated, may hold values from -0.125 to 0.125
- decay_lowrank_output: bfloat16 [64, 2048], replicated, may hold values from -0.75 to 0.75
- decay_base_preact: float32 [2048], replicated, may hold values from -6 to -1
- context_rate_input: bfloat16 [2048, 64], replicated, may hold values from -0.125 to 0.125
- context_rate_output: bfloat16 [64, 2048], replicated, may hold values from -0.75 to 0.75
- context_rate_base: float32 [2048], replicated, may hold values from -4 to 4
- removal_key_scale: float32 [2048], replicated, may hold values from 0.1 to 1.9
- key_context_rate_blend: float32 [2048], replicated, may hold values from 0.1 to 1.9
- present_item_coefficient: float32 [32, 64], replicated, may hold values from -0.9 to 0.9
- head_norm_gain: float32 [2048], replicated, may hold values from 0.1 to 1.9
- mixer_output_matrix: bfloat16 [2048, 2048], P(None, 'ep'), may hold values from -0.125 to 0.125
- mixer_norm_gain: float32 [2048], replicated, may hold values from 0.1 to 1.9
- group_router_columns: bfloat16 [2048, 4], replicated, may hold values from -8 to 8
- expert_router_columns: bfloat16 [2048, 16], replicated, may hold values from -0.125 to 0.125
- expert_gate_matrix: bfloat16 [16, 2048, 256], P('ep'), may hold values from -0.125 to 0.125
- expert_up_matrix: bfloat16 [16, 2048, 256], P('ep'), may hold values from -0.125 to 0.125
- expert_down_matrix: bfloat16 [16, 256, 2048], P('ep'), may hold values from -0.375 to 0.375
- final_norm_gain: float32 [2048], replicated, may hold values from 0.1 to 1.9
- routes: int32 [224, 4], P(('grp', 'ep')), parts along dimension 0, may hold values from 0 to 15, as said below
Outputs:
- tokens_out: bfloat16 [224, 2048], P(('grp', 'ep')), parts along dimension 0
- next_recurrent_state: float32 [224, 32, 64, 64], P(('grp', 'ep')), parts along dimension 0
The draws below stay inside these ranges and needn't reach their ends.
There are 2 independent parts, one for each index of `grp`. The reference program is written for one: setup_inputs(seed, part) draws one part's arguments, and reference() takes and returns one part's arrays. A program takes and returns all parts, laid end to end along the dimension named above; an argument that names none is the same for every part. Nothing has to cross between parts.
Inputs may be any that keep to these rules, and one draw needn't show every extreme that they name: `routes`: the 4 experts of a row are different and lie in the same group (expert // 4). In each aligned block of 7 rows (the rows of one device) no expert is named more than 2 times, and in every block some expert is named exactly 2 times.
All inputs are finite; a program needn't handle non-finite values.
Results may differ from the reference program's by a relative error of at most 0.0067.
Values may be sent and summed in bfloat16 or wider, within the bound.
A program may use at most 128 MiB of HBM per device.

```python
import jax
import jax.numpy as jnp
from jax import lax

D = 2048
MIXER_HEADS = 32
HEAD_WIDTH = 64
LD = 64
LA = 64
FFE = 256
GROUPS = 4
TOP_E = 4
CAP = 2
SEQ_DEV = 7
EXPERTS = 16
TOKENS = 112
SLOTS = 32


def draw_group_router_columns(key, part):
    base = jax.random.normal(key, (D, GROUPS), jnp.float32) * D ** (-0.5)
    return jnp.clip(base, -8.0, 8.0).astype(jnp.bfloat16)


def draw_routes(key, part):
    per_group = EXPERTS // GROUPS
    stride = TOP_E // CAP
    steps_group = per_group // stride
    tickets = GROUPS * steps_group
    hot_group = jax.random.randint(jax.random.fold_in(key, 11), (), 0, GROUPS, dtype=jnp.int32)
    hot_offset = jax.random.randint(jax.random.fold_in(key, 12), (), 0, per_group, dtype=jnp.int32)
    popular = jax.random.permutation(jax.random.fold_in(key, 13), GROUPS).astype(jnp.int32)
    block_keys = jax.random.split(jax.random.fold_in(key, 14), TOKENS // SEQ_DEV)
    within = jnp.arange(TOP_E, dtype=jnp.int32)

    def one_block(block_key):
        order_key = jax.random.fold_in(block_key, 1)
        score_key = jax.random.fold_in(block_key, 2)
        offset_key = jax.random.fold_in(block_key, 3)
        row_order = jax.random.permutation(order_key, SEQ_DEV).astype(jnp.int32)
        ticket_ids = jnp.arange(tickets, dtype=jnp.int32)
        ticket_group = ticket_ids // steps_group
        ticket_step = ticket_ids % steps_group
        scores = jax.random.randint(score_key, (tickets,), 0, 4096, dtype=jnp.int32) + popular[ticket_group] * 1024
        banned = (ticket_group == hot_group) & (ticket_step < 2)
        scores = jnp.where(banned, -65536, scores) * tickets + ticket_ids
        _, picked = lax.top_k(scores, SEQ_DEV)
        hot_pair = jnp.stack([hot_group * steps_group, hot_group * steps_group + 1]).astype(jnp.int32)
        chosen = jnp.concatenate([hot_pair, picked[:SEQ_DEV - 2].astype(jnp.int32)])
        row_ticket = chosen[row_order]
        group_id = row_ticket // steps_group
        step_id = row_ticket % steps_group
        offset = jax.random.randint(offset_key, (GROUPS,), 0, per_group, dtype=jnp.int32)
        offset = jnp.where(jnp.arange(GROUPS, dtype=jnp.int32) == hot_group, hot_offset, offset)
        place = (offset[group_id][:, None] + step_id[:, None] * stride + within[None, :]) % per_group
        return group_id[:, None] * per_group + place
    return jax.vmap(one_block)(block_keys).reshape(TOKENS, TOP_E).astype(jnp.int32)


def level_of(stream_key, dims, cuts, low, high):
    def one(position, blocks):
        draws = jax.random.uniform(jax.random.fold_in(jax.random.fold_in(stream_key, 6), position), (blocks,), jnp.float32, low / len(cuts), high / len(cuts))
        return jnp.repeat(jnp.exp(draws), dims[position] // blocks).reshape((-1,) + (1,) * (len(dims) - position - 1))

    level = one(*cuts[0])
    for cut in cuts[1:]:
        level = level * one(*cut)
    return level


def normal_values(stream_key, shape, scale, bound, pieces=(), held_as=jnp.bfloat16):
    gain = level_of(stream_key, shape, pieces, -0.22, 0.18) if pieces else 1.0
    drawn = jax.random.normal(stream_key, shape, jnp.float32) * scale * gain
    return jnp.minimum(jnp.maximum(drawn, -bound), bound).astype(held_as)


def setup_inputs(seed: int = 0, part: int = 0) -> dict:
    splits = jax.random.split(jax.random.key(seed), 25)
    part_splits = jax.random.split(jax.random.fold_in(splits[24], part), 25)
    sequence_input_rows = normal_values(part_splits[0], (TOKENS, D), 1.0, 6.0, ((0, 16),))
    value_key_state = normal_values(part_splits[1], (TOKENS, MIXER_HEADS, HEAD_WIDTH, HEAD_WIDTH), 0.5, 4.0, ((0, 16),), jnp.float32)
    receptance_matrix = normal_values(splits[2], (D, MIXER_HEADS * HEAD_WIDTH), D ** -0.5, 0.125, ((1, 16),))
    key_matrix = normal_values(splits[3], (D, MIXER_HEADS * HEAD_WIDTH), D ** -0.5, 0.125, ((1, 16),))
    value_matrix = normal_values(splits[4], (D, MIXER_HEADS * HEAD_WIDTH), D ** -0.5, 0.125, ((1, 16),))
    decay_lowrank_input = normal_values(splits[5], (D, LD), D ** -0.5, 0.125)
    decay_lowrank_output = normal_values(splits[6], (LD, MIXER_HEADS * HEAD_WIDTH), (1.5 * LD ** -0.5), 0.75)
    decay_base_preact = jnp.clip(jax.random.uniform(splits[7], (MIXER_HEADS * HEAD_WIDTH,), jnp.float32, -6.0, -1.0), -6.0, -1.0)
    context_rate_input = normal_values(splits[8], (D, LA), D ** -0.5, 0.125)
    context_rate_output = normal_values(splits[9], (LA, MIXER_HEADS * HEAD_WIDTH), LA ** -0.5, 0.75)
    context_rate_base = normal_values(splits[10], (MIXER_HEADS * HEAD_WIDTH,), 1.0, 4.0, (), jnp.float32)
    removal_key_scale = jnp.clip(1.0 + 0.18 * jax.random.normal(splits[11], (MIXER_HEADS * HEAD_WIDTH,), jnp.float32), 0.1, 1.9)
    key_context_rate_blend = jnp.clip(1.0 + 0.18 * jax.random.normal(splits[12], (MIXER_HEADS * HEAD_WIDTH,), jnp.float32), 0.1, 1.9)
    present_item_coefficient = normal_values(splits[13], (MIXER_HEADS, HEAD_WIDTH), 0.15, 0.9, (), jnp.float32)
    head_norm_gain = jnp.clip(1.0 + 0.18 * jax.random.normal(splits[14], (MIXER_HEADS * HEAD_WIDTH,), jnp.float32), 0.1, 1.9)
    mixer_output_matrix = normal_values(splits[15], (MIXER_HEADS * HEAD_WIDTH, D), (MIXER_HEADS * HEAD_WIDTH) ** -0.5, 0.125, ((1, 16),))
    mixer_norm_gain = jnp.clip(1.0 + 0.18 * jax.random.normal(splits[16], (D,), jnp.float32), 0.1, 1.9)
    group_router_columns = draw_group_router_columns(jax.random.fold_in(splits[24], 71), part)
    expert_router_columns = normal_values(splits[18], (D, EXPERTS), D ** -0.5, 0.125)
    expert_gate_matrix = normal_values(splits[19], (EXPERTS, D, FFE), D ** -0.5, 0.125, ((0, 16),))
    expert_up_matrix = normal_values(splits[20], (EXPERTS, D, FFE), D ** -0.5, 0.125, ((0, 16),))
    expert_down_matrix = normal_values(splits[21], (EXPERTS, FFE, D), FFE ** -0.5, 0.375, ((0, 16),))
    final_norm_gain = jnp.clip(1.0 + 0.18 * jax.random.normal(splits[22], (D,), jnp.float32), 0.1, 1.9)
    routes = draw_routes(jax.random.fold_in(jax.random.fold_in(splits[24], part), 71), part)
    return dict(sequence_input_rows=sequence_input_rows, value_key_state=value_key_state, receptance_matrix=receptance_matrix, key_matrix=key_matrix, value_matrix=value_matrix, decay_lowrank_input=decay_lowrank_input, decay_lowrank_output=decay_lowrank_output, decay_base_preact=decay_base_preact, context_rate_input=context_rate_input, context_rate_output=context_rate_output, context_rate_base=context_rate_base, removal_key_scale=removal_key_scale, key_context_rate_blend=key_context_rate_blend, present_item_coefficient=present_item_coefficient, head_norm_gain=head_norm_gain, mixer_output_matrix=mixer_output_matrix, mixer_norm_gain=mixer_norm_gain, group_router_columns=group_router_columns, expert_router_columns=expert_router_columns, expert_gate_matrix=expert_gate_matrix, expert_up_matrix=expert_up_matrix, expert_down_matrix=expert_down_matrix, final_norm_gain=final_norm_gain, routes=routes)


residual_scale = 8.0 ** 0.25
norm_eps = 1e-05
group_eps = 0.00064

def layer_norm(values, norm_gain):
    center = lax.optimization_barrier(jnp.mean(values, -1, keepdims=True))
    spread = lax.optimization_barrier(jnp.mean(jnp.square(values - center), -1, keepdims=True))
    return (values - center) * lax.rsqrt(spread + norm_eps) * norm_gain

def token_mixer_step(sequence_input_rows, receptance_rows, key_projected_rows, value_projected_rows, value_key_state, decay_lowrank_input, decay_lowrank_output, decay_base_preact, context_rate_input, context_rate_output, context_rate_base, removal_key_scale, key_context_rate_blend, present_item_coefficient, head_norm_gain):
    series_entry_number = sequence_input_rows.shape[0]
    attention_subspace_number, subspace_dimension = present_item_coefficient.shape
    decay_low = jnp.tanh(jnp.dot(sequence_input_rows, decay_lowrank_input, preferred_element_type=jnp.float32)).astype(jnp.bfloat16)
    decay_pre = decay_base_preact + jnp.dot(decay_low, decay_lowrank_output, preferred_element_type=jnp.float32)
    log_rate = -jax.nn.softplus(-decay_pre) - 0.5
    decay = jnp.exp(-jnp.exp(log_rate))
    iclr_low = jnp.dot(sequence_input_rows, context_rate_input, preferred_element_type=jnp.float32).astype(jnp.bfloat16)
    iclr_rate = jax.nn.sigmoid(context_rate_base + jnp.dot(iclr_low, context_rate_output, preferred_element_type=jnp.float32))

    def to_heads(values):
        return values.astype(jnp.float32).reshape(series_entry_number, attention_subspace_number, subspace_dimension)
    acceptance_subspaces = to_heads(receptance_rows)
    key_heads = to_heads(key_projected_rows)
    content_subspace_entries = to_heads(value_projected_rows)
    decay_heads = to_heads(decay)
    rate_heads = to_heads(iclr_rate)
    scaled_key = key_heads * removal_key_scale.reshape(attention_subspace_number, subspace_dimension)
    removal_dir = scaled_key * lax.rsqrt(lax.optimization_barrier(jnp.sum(scaled_key * scaled_key, -1, keepdims=True)) + 1e-06)
    adjusted_lookup_vector = key_heads * (1.0 + (rate_heads - 1.0) * key_context_rate_blend.reshape(attention_subspace_number, subspace_dimension))
    removed = jnp.einsum('bhvk,bhk->bhv', value_key_state, removal_dir, precision=lax.Precision.HIGHEST)
    next_recurrent_state = value_key_state * decay_heads[:, :, None, :] - removed[..., None] * (removal_dir * rate_heads)[:, :, None, :] + content_subspace_entries[..., None] * adjusted_lookup_vector[:, :, None, :]
    readout = jnp.einsum('bhvk,bhk->bhv', next_recurrent_state, acceptance_subspaces, precision=lax.Precision.HIGHEST)
    center = lax.optimization_barrier(jnp.mean(readout, -1, keepdims=True))
    spread = lax.optimization_barrier(jnp.mean(jnp.square(readout - center), -1, keepdims=True))
    standardized_entries = (readout - center) * lax.rsqrt(spread + group_eps) * head_norm_gain.reshape(attention_subspace_number, subspace_dimension)
    present_extra_reward = lax.optimization_barrier(jnp.sum(acceptance_subspaces * adjusted_lookup_vector * present_item_coefficient, -1, keepdims=True)) * content_subspace_entries
    attention_mixing_outcome = (standardized_entries + present_extra_reward).reshape(series_entry_number, attention_subspace_number * subspace_dimension).astype(jnp.bfloat16)
    return (attention_mixing_outcome, next_recurrent_state)

def routing_gate(hidden, route_rows, chosen, group_router_columns, expert_router_columns):
    group_count = group_router_columns.shape[1]
    expert_count = expert_router_columns.shape[1]
    per_group = expert_count // group_count
    group_logits = jnp.dot(hidden, group_router_columns, preferred_element_type=jnp.float32)
    expert_logits = jnp.dot(hidden, expert_router_columns, preferred_element_type=jnp.float32)
    largest = lax.optimization_barrier(jnp.max(group_logits, -1, keepdims=True))
    lifted = jnp.exp(group_logits - largest)
    in_group = (chosen // per_group)[:, None] == jnp.arange(group_count, dtype=jnp.int32)[None, :]
    group_prob = lax.optimization_barrier(jnp.sum(jnp.where(in_group, lifted, 0.0), -1)) / lax.optimization_barrier(jnp.sum(lifted, -1))
    columns = jnp.arange(expert_count, dtype=jnp.int32)[None, :]
    chosen_logit = lax.optimization_barrier(jnp.sum(jnp.where(chosen[:, None] == columns, expert_logits, 0.0), -1))
    total = jnp.zeros_like(chosen_logit)
    for slot in range(route_rows.shape[1]):
        other_logit = lax.optimization_barrier(jnp.sum(jnp.where(route_rows[:, slot][:, None] == columns, expert_logits, 0.0), -1))
        total = total + jnp.exp(other_logit - chosen_logit)
    return group_prob / total

def expert_mlp(inputs, gate_weight, up_weight, down_weight):
    gate_part = jnp.dot(inputs, gate_weight, preferred_element_type=jnp.float32)
    up_part = jnp.dot(inputs, up_weight, preferred_element_type=jnp.float32)
    act = (jax.nn.silu(gate_part) * up_part).astype(jnp.bfloat16)
    return jnp.dot(act, down_weight, preferred_element_type=jnp.float32).astype(jnp.bfloat16)

def reference(sequence_input_rows, value_key_state, receptance_matrix, key_matrix, value_matrix, decay_lowrank_input, decay_lowrank_output, decay_base_preact, context_rate_input, context_rate_output, context_rate_base, removal_key_scale, key_context_rate_blend, present_item_coefficient, head_norm_gain, mixer_output_matrix, mixer_norm_gain, group_router_columns, expert_router_columns, expert_gate_matrix, expert_up_matrix, expert_down_matrix, final_norm_gain, routes):

    def apply_projection(weight):
        return jnp.dot(sequence_input_rows, weight, preferred_element_type=jnp.float32).astype(jnp.bfloat16)
    attention_mixing_outcome, next_recurrent_state = token_mixer_step(sequence_input_rows, apply_projection(receptance_matrix), apply_projection(key_matrix), apply_projection(value_matrix), value_key_state, decay_lowrank_input, decay_lowrank_output, decay_base_preact, context_rate_input, context_rate_output, context_rate_base, removal_key_scale, key_context_rate_blend, present_item_coefficient, head_norm_gain)
    attn_out = jnp.dot(attention_mixing_outcome, mixer_output_matrix, preferred_element_type=jnp.float32).astype(jnp.bfloat16)
    hidden = layer_norm(residual_scale * sequence_input_rows.astype(jnp.float32) + attn_out.astype(jnp.float32), mixer_norm_gain).astype(jnp.bfloat16)
    gate_values = jnp.stack([routing_gate(hidden, routes, routes[:, slot], group_router_columns, expert_router_columns) for slot in range(routes.shape[1])], 1)
    token_total = hidden.shape[0]

    def per_expert(running, expert_id):
        is_named = routes == expert_id
        weight_row = lax.optimization_barrier(jnp.sum(jnp.where(is_named, gate_values, 0.0), 1))
        routed = jnp.any(is_named, 1)
        index_list = jnp.nonzero(routed, size=SLOTS, fill_value=0)[0].astype(jnp.int32)
        filled = jnp.arange(SLOTS, dtype=jnp.int32) < jnp.sum(routed.astype(jnp.int32))
        outputs = expert_mlp(hidden[index_list], expert_gate_matrix[expert_id], expert_up_matrix[expert_id], expert_down_matrix[expert_id])
        scaled = jnp.where(filled[:, None], weight_row[index_list][:, None] * outputs.astype(jnp.float32), 0.0)
        return (running.at[index_list].add(scaled), None)
    expert_sum, _ = lax.scan(per_expert, jnp.zeros((token_total, D), jnp.float32), jnp.arange(EXPERTS, dtype=jnp.int32))
    tokens_out = layer_norm(residual_scale * hidden.astype(jnp.float32) + expert_sum, final_norm_gain).astype(jnp.bfloat16)
    return (tokens_out, next_recurrent_state)
```

```python
import functools

import jax
import jax.numpy as jnp
from jax import lax
from jax.experimental import pallas as pl
from jax.experimental.pallas import tpu as pltpu
from jax.sharding import PartitionSpec as P

CAP = 2
PAD = 8
LANES = 128

residual_scale = 8.0**0.25
norm_eps = 1e-05
group_eps = 0.00064

MESH = pl.DeviceIdType.MESH
F32 = jnp.float32
BF16 = jnp.bfloat16
HIGHEST = lax.Precision.HIGHEST


def layer_norm(values, norm_gain):
    center = jnp.mean(values, -1, keepdims=True)
    spread = jnp.mean(jnp.square(values - center), -1, keepdims=True)
    return (values - center) * lax.rsqrt(spread + norm_eps) * norm_gain


def contract(a, b, dims, precision=None):
    return lax.dot_general(a, b, ((dims[:1], dims[1:]), ((), ())), precision=precision,
                           preferred_element_type=F32)


def sigmoid(values):
    return 1.0 / (1.0 + jnp.exp(-values))


def each_peer(n, me, act):
    def body(d, carry):
        act(lax.rem(me + d, n))
        return carry

    lax.fori_loop(1, n, body, 0)


def enter(n, me):
    barrier = pltpu.get_barrier_semaphore()
    each_peer(n, me, lambda peer: pl.semaphore_signal(
        barrier, inc=1, device_id={"ep": peer}, device_id_type=MESH))
    pl.semaphore_wait(barrier, n - 1)


class Exchange:
    def __init__(self, n, me, source_of, landing, send, recv):
        self.n, self.me, self.source_of = n, me, source_of
        self.landing, self.send, self.recv = landing, send, recv

    def start(self, peer):
        pltpu.make_async_remote_copy(
            src_ref=self.source_of(peer),
            dst_ref=self.landing.at[self.me],
            send_sem=self.send.at[peer],
            recv_sem=self.recv.at[self.me],
            device_id={"ep": peer},
            device_id_type=MESH,
        ).start()

    def start_all(self):
        each_peer(self.n, self.me, self.start)

    def incoming(self, peer):
        return pltpu.make_async_remote_copy(
            src_ref=self.source_of(peer),
            dst_ref=self.landing.at[peer],
            send_sem=self.send.at[peer],
            recv_sem=self.recv.at[peer],
            device_id={"ep": peer},
            device_id_type=MESH,
        )

    def wait_recv(self, then=None):
        def body(d, carry):
            peer = lax.rem(self.me + self.n - d, self.n)
            self.incoming(peer).wait_recv()
            if then is not None:
                then(peer)
            return carry

        lax.fori_loop(1, self.n, body, 0)

    def wait_send(self):
        each_peer(self.n, self.me, lambda peer: self.incoming(peer).wait_send())


def project_kernel(
    n, x_ref, wr, wk, wv, dli, dlo, dbase, cri, cro, cbase,
    rkv_out, decay_out, rate_out,
    weights, dli_v, dlo_v, cri_v, cro_v, gathered, rows, outs, back,
    local, send1, recv1, send2, recv2,
):
    me = lax.axis_index("ep")
    series, _ = x_ref.shape
    width = wr.shape[1]
    loads = [
        pltpu.make_async_copy(src, dst, local.at[i])
        for i, (src, dst) in enumerate([
            (dli, dli_v), (cri, cri_v), (dlo, dlo_v), (cro, cro_v),
            (wr, weights.at[0]), (wk, weights.at[1]), (wv, weights.at[2]),
        ])
    ]
    for load in loads:
        load.start()
    enter(n, me)
    gather = Exchange(n, me, lambda peer: x_ref, gathered, send1, recv1)
    gather.start_all()

    rows[...] = jnp.zeros_like(rows)

    def place(source, block):
        rows[pl.ds(pl.multiple_of(source * PAD, PAD), series), :] = block.astype(F32)

    place(me, x_ref[...])
    own = rows[pl.ds(pl.multiple_of(me * PAD, PAD), PAD), :].astype(BF16)
    for load in loads[:4]:
        load.wait()
    decay_low = jnp.tanh(contract(own, dli_v[...], (1, 1))).astype(BF16)
    decay_pre = dbase[...] + contract(decay_low, dlo_v[...], (1, 0))
    decay_out[...] = jnp.exp(sigmoid(decay_pre) * -(2.718281828459045**-0.5))
    iclr_low = contract(own, cri_v[...], (1, 1)).astype(BF16)
    rate_out[...] = sigmoid(cbase[...] + contract(iclr_low, cro_v[...], (1, 0)))
    for load in loads[4:]:
        load.wait()

    gather.wait_recv(lambda peer: place(peer, gathered[peer]))
    lhs = rows[...].astype(BF16)
    for c in range(3):
        columns = jnp.dot(lhs, weights[c], preferred_element_type=F32)
        outs[:, c] = columns.reshape(n, PAD, width).astype(BF16)
    spread = Exchange(n, me, lambda peer: outs.at[peer], back, send2, recv2)
    spread.start_all()
    back[me] = outs[me]
    spread.wait_recv()
    for source in range(n):
        for c in range(3):
            rkv_out[c, :, source * width : (source + 1) * width] = back[source, c].astype(F32)
    gather.wait_send()
    spread.wait_send()


def mixer_kernel(
    state, rkv, decay_ref, rate_ref, scale_ref, blend_ref, coef_ref, gain_ref,
    mixed_out, next_out,
):
    step = pl.program_id(0)
    series, per_step, head, _ = state.shape
    value_columns = jnp.transpose(rkv[2])
    lane = lax.broadcasted_iota(jnp.int32, (head, LANES), 1)
    pieces = []
    for h in range(per_step):
        part = slice(h * head, (h + 1) * head)
        r, k, v = (rkv[c][:, part] for c in range(3))
        decay, rate = decay_ref[:, part], rate_ref[:, part]
        scaled = k * scale_ref[:, part]
        removal = scaled * lax.rsqrt(jnp.sum(scaled * scaled, -1, keepdims=True) + 1e-06)
        key_mod = k * (1.0 + (rate - 1.0) * blend_ref[:, part])
        written = removal * rate
        readouts = jnp.zeros((head, LANES), F32)
        for t in range(series):
            row = slice(t, t + 1)
            block = state[t, h]
            removed = jnp.sum(block * removal[row], -1, keepdims=True)
            after = (
                block * decay[row]
                - removed * written[row]
                + value_columns[part, row] * key_mod[row]
            )
            next_out[t, h] = after
            readout = jnp.sum(after * r[row], -1, keepdims=True)
            readouts = jnp.where(lane == t, readout, readouts)
        readout = jnp.transpose(readouts)[:PAD]
        center = jnp.mean(readout, -1, keepdims=True)
        spread = jnp.mean(jnp.square(readout - center), -1, keepdims=True)
        standard = (readout - center) * lax.rsqrt(spread + group_eps) * gain_ref[:, part]
        coef = coef_ref[pl.ds(step * per_step + h, 1), :]
        present = jnp.sum(r * key_mod * coef, -1, keepdims=True) * v
        pieces.append(standard + present)
    mixed_out[...] = jnp.concatenate(pieces, axis=1).astype(BF16)


def finish_kernel(
    n, mixed, x_ref, routes, norm_gain, group_router, expert_router, final_gain,
    w_out, w_gate, w_up, w_down,
    tokens_out,
    wo_v, wg_v, wu_v, wd_v, gathered, outs, back, attn, resid, flat, away, arrived, home,
    landed, local, send1, recv1, send2, recv2, send3, recv3, send4, recv4,
):
    me = lax.axis_index("ep")
    series, model = x_ref.shape
    width = w_out.shape[1]
    experts = expert_router.shape[0]
    groups = group_router.shape[0]
    top = routes.shape[0]
    loads = [
        pltpu.make_async_copy(src, dst, local.at[i])
        for i, (src, dst) in enumerate(
            [(w_out, wo_v), (w_gate, wg_v), (w_up, wu_v), (w_down, wd_v)]
        )
    ]
    for load in loads:
        load.start()
    enter(n, me)
    gather = Exchange(n, me, lambda peer: mixed, gathered, send1, recv1)
    gather.start_all()
    gathered[me] = mixed[...]
    resid[...] = jnp.zeros_like(resid)
    resid[:series, :] = x_ref[...].astype(F32)

    slots = experts * CAP
    slot_ids = lax.broadcasted_iota(jnp.int32, (slots, PAD), 0)
    named = jnp.zeros((slots, PAD), F32)
    rank = jnp.zeros((slots, PAD), F32)
    for k in range(top):
        offset = slot_ids - routes[k : k + 1, :] * CAP
        match = (offset >= 0) & (offset < CAP)
        named = named + jnp.where(match, 1.0, 0.0)
        rank = rank + jnp.where(match, offset.astype(F32), 0.0)
    earlier = (
        lax.broadcasted_iota(jnp.int32, (PAD, PAD), 0)
        < lax.broadcasted_iota(jnp.int32, (PAD, PAD), 1)
    ).astype(F32)
    before = contract(named, earlier, (1, 0))
    placing = jnp.where(jnp.abs(before - rank) < 0.5, named, 0.0)
    ahead = lax.broadcasted_iota(jnp.int32, (slots, experts), 0) - CAP * (
        lax.broadcasted_iota(jnp.int32, (slots, experts), 1)
    )
    repeat = jnp.where((ahead >= 0) & (ahead < CAP), 1.0, 0.0)

    loads[0].wait()
    gather.wait_recv()
    lhs = gathered[...].astype(F32).reshape(n * PAD, model).astype(BF16)
    columns = jnp.dot(lhs, wo_v[...], preferred_element_type=F32)
    outs[...] = columns.reshape(n, PAD, width).astype(BF16)
    spread = Exchange(n, me, lambda peer: outs.at[peer], back, send2, recv2)
    spread.start_all()
    back[me] = outs[me]
    spread.wait_recv()
    for source in range(n):
        attn[:, source * width : (source + 1) * width] = back[source].astype(F32)
    hidden = layer_norm(residual_scale * resid[...] + attn[...], norm_gain[...]).astype(BF16)

    flat[...] = contract(placing.astype(BF16), hidden, (1, 0))

    for e in range(n):
        away[e] = flat[e * CAP : (e + 1) * CAP, :].astype(BF16)
    dispatch = Exchange(n, me, lambda peer: away.at[peer], arrived, send3, recv3)
    dispatch.start_all()
    arrived[me] = away[me]

    group_logits = contract(group_router[...], hidden, (1, 1))
    expert_logits = contract(
        repeat, contract(expert_router[...], hidden, (1, 1)), (1, 0), HIGHEST
    )
    lifted = jnp.exp(group_logits - jnp.max(group_logits, 0, keepdims=True))
    group_ids = lax.broadcasted_iota(jnp.int32, (groups, PAD), 0) * (experts // groups)
    first = routes[0:1, :]
    in_group = (first >= group_ids) & (first < group_ids + experts // groups)
    group_prob = jnp.sum(jnp.where(in_group, lifted, 0.0), 0, keepdims=True) / jnp.sum(
        lifted, 0, keepdims=True
    )
    is_named = named > 0.5
    highest = jnp.max(jnp.where(is_named, expert_logits, -1e30), 0, keepdims=True)
    raised = jnp.where(is_named, jnp.exp(expert_logits - highest), 0.0)
    total = jnp.sum(raised, 0, keepdims=True) / CAP
    gates = group_prob * raised / jnp.where(total > 0.0, total, 1.0)
    weights = gates * placing

    for load in loads[1:]:
        load.wait()

    dispatch.wait_recv()
    for s in range(n):
        flat[s * CAP : (s + 1) * CAP, :] = arrived[s].astype(F32)
    rows = flat[...].astype(BF16)
    gate_part = jnp.dot(rows, wg_v[0], preferred_element_type=F32)
    up_part = jnp.dot(rows, wu_v[0], preferred_element_type=F32)
    act = (gate_part * sigmoid(gate_part) * up_part).astype(BF16)
    flat[...] = jnp.dot(act, wd_v[0], preferred_element_type=F32)

    for s in range(n):
        home[s] = flat[s * CAP : (s + 1) * CAP, :].astype(BF16)
    giveback = Exchange(n, me, lambda peer: home.at[peer], landed, send4, recv4)
    giveback.start_all()
    landed[me] = home[me]

    giveback.wait_recv()
    for e in range(n):
        flat[e * CAP : (e + 1) * CAP, :] = landed[e].astype(F32)
    expert_sum = contract(weights, flat[...], (0, 0), HIGHEST)
    tokens = layer_norm(residual_scale * hidden.astype(F32) + expert_sum, final_gain[...])
    tokens_out[...] = tokens[:series].astype(BF16)
    gather.wait_send()
    spread.wait_send()
    dispatch.wait_send()
    giveback.wait_send()


VMEM = pl.BlockSpec(memory_space=pltpu.VMEM)
ANY = pl.BlockSpec(memory_space=pl.ANY)
MIB = 1024 * 1024


def on_device(
    n,
    sequence_input_rows,
    value_key_state,
    receptance_matrix,
    key_matrix,
    value_matrix,
    decay_lowrank_input,
    decay_lowrank_output,
    decay_base_preact,
    context_rate_input,
    context_rate_output,
    context_rate_base,
    removal_key_scale,
    key_context_rate_blend,
    present_item_coefficient,
    head_norm_gain,
    mixer_output_matrix,
    mixer_norm_gain,
    group_router_columns,
    expert_router_columns,
    expert_gate_matrix,
    expert_up_matrix,
    expert_down_matrix,
    final_norm_gain,
    routes,
):
    series, model = sequence_input_rows.shape
    heads, head = present_item_coefficient.shape
    inner = heads * head
    width = receptance_matrix.shape[1]
    out_width = mixer_output_matrix.shape[1]
    experts = expert_router_columns.shape[1]
    low_d, low_a = decay_lowrank_input.shape[1], context_rate_input.shape[1]
    hidden_units = expert_gate_matrix.shape[2]
    assert experts == n

    def row(values):
        return values.reshape(1, -1)

    dma = pltpu.SemaphoreType.DMA
    rkv, decay, rate = pl.pallas_call(
        functools.partial(project_kernel, n),
        out_shape=[
            jax.ShapeDtypeStruct((3, PAD, inner), F32),
            jax.ShapeDtypeStruct((PAD, inner), F32),
            jax.ShapeDtypeStruct((PAD, inner), F32),
        ],
        in_specs=[VMEM, ANY, ANY, ANY, ANY, ANY, VMEM, ANY, ANY, VMEM],
        out_specs=[VMEM] * 3,
        scratch_shapes=[
            pltpu.VMEM((3, model, width), BF16),
            pltpu.VMEM((low_d, model), BF16),
            pltpu.VMEM((low_d, inner), BF16),
            pltpu.VMEM((low_a, model), BF16),
            pltpu.VMEM((low_a, inner), BF16),
            pltpu.VMEM((n, series, model), BF16),
            pltpu.VMEM((n * PAD, model), F32),
            pltpu.VMEM((n, 3, PAD, width), BF16),
            pltpu.VMEM((n, 3, PAD, width), BF16),
            dma((7,)),
        ]
        + [dma((n,))] * 4,
        compiler_params=pltpu.CompilerParams(
            collective_id=0, has_side_effects=True, vmem_limit_bytes=32 * MIB
        ),
        name="project",
    )(
        sequence_input_rows,
        receptance_matrix,
        key_matrix,
        value_matrix,
        decay_lowrank_input.T,
        decay_lowrank_output,
        row(decay_base_preact),
        context_rate_input.T,
        context_rate_output,
        row(context_rate_base),
    )

    per_step = LANES // head

    def lanes(rows):
        return pl.BlockSpec((rows, LANES), lambda s: (0, s))

    state_spec = pl.BlockSpec((series, per_step, head, head), lambda s: (0, s, 0, 0))
    mixed, next_recurrent_state = pl.pallas_call(
        mixer_kernel,
        grid=(heads // per_step,),
        out_shape=[
            jax.ShapeDtypeStruct((PAD, inner), BF16),
            jax.ShapeDtypeStruct(value_key_state.shape, F32),
        ],
        in_specs=[
            state_spec,
            pl.BlockSpec((3, PAD, LANES), lambda s: (0, 0, s)),
            lanes(PAD),
            lanes(PAD),
            lanes(1),
            lanes(1),
            pl.BlockSpec((heads, head), lambda s: (0, 0)),
            lanes(1),
        ],
        out_specs=[lanes(PAD), state_spec],
        name="mixer",
    )(
        value_key_state,
        rkv,
        decay,
        rate,
        row(removal_key_scale),
        row(key_context_rate_blend),
        present_item_coefficient,
        row(head_norm_gain),
    )

    routes_t = jnp.pad(routes.T, ((0, 0), (0, PAD - series)), constant_values=-1)
    tokens_out = pl.pallas_call(
        functools.partial(finish_kernel, n),
        out_shape=jax.ShapeDtypeStruct((series, model), BF16),
        in_specs=[VMEM] * 7 + [ANY] * 4,
        out_specs=VMEM,
        scratch_shapes=[
            pltpu.VMEM((inner, out_width), BF16),
            pltpu.VMEM((1, model, hidden_units), BF16),
            pltpu.VMEM((1, model, hidden_units), BF16),
            pltpu.VMEM((1, hidden_units, model), BF16),
            pltpu.VMEM((n, PAD, inner), BF16),
            pltpu.VMEM((n, PAD, out_width), BF16),
            pltpu.VMEM((n, PAD, out_width), BF16),
            pltpu.VMEM((PAD, model), F32),
            pltpu.VMEM((PAD, model), F32),
            pltpu.VMEM((experts * CAP, model), F32),
        ]
        + [pltpu.VMEM((n, CAP, model), BF16)] * 4
        + [dma((4,))]
        + [dma((n,))] * 8,
        compiler_params=pltpu.CompilerParams(
            collective_id=1, has_side_effects=True, vmem_limit_bytes=32 * MIB
        ),
        name="finish",
    )(
        mixed,
        sequence_input_rows,
        routes_t,
        row(mixer_norm_gain),
        group_router_columns.T,
        expert_router_columns.T,
        row(final_norm_gain),
        mixer_output_matrix,
        expert_gate_matrix,
        expert_up_matrix,
        expert_down_matrix,
    )
    return (tokens_out, next_recurrent_state)


def solution(mesh):
    in_specs = (
        P(("grp", "ep"), None),
        P(("grp", "ep"), None, None, None),
        P(None, "ep"),
        P(None, "ep"),
        P(None, "ep"),
        P(),
        P(),
        P(),
        P(),
        P(),
        P(),
        P(),
        P(),
        P(),
        P(),
        P(None, "ep"),
        P(),
        P(),
        P(),
        P("ep", None, None),
        P("ep", None, None),
        P("ep", None, None),
        P(),
        P(("grp", "ep"), None),
    )
    out_specs = (P(("grp", "ep"), None), P(("grp", "ep"), None, None, None))
    return jax.shard_map(
        functools.partial(on_device, mesh.shape["ep"]),
        mesh=mesh, in_specs=in_specs, out_specs=out_specs, check_vma=False,
    )
```

```python
import functools

import jax
import jax.numpy as jnp
from jax import lax
from jax.experimental import pallas as pl
from jax.experimental.pallas import tpu as pltpu
from jax.sharding import PartitionSpec as P

CAP = 2
PAD = 8
LANES = 128

residual_scale = 8.0**0.25
norm_eps = 1e-05
group_eps = 0.00064

MESH = pl.DeviceIdType.MESH
F32 = jnp.float32
BF16 = jnp.bfloat16
HIGHEST = lax.Precision.HIGHEST


def layer_norm(values, norm_gain):
    center = jnp.mean(values, -1, keepdims=True)
    spread = jnp.mean(jnp.square(values - center), -1, keepdims=True)
    return (values - center) * lax.rsqrt(spread + norm_eps) * norm_gain


def contract(a, b, dims, precision=None):
    return lax.dot_general(a, b, ((dims[:1], dims[1:]), ((), ())), precision=precision,
                           preferred_element_type=F32)


def sigmoid(values):
    return 1.0 / (1.0 + jnp.exp(-values))


def each_peer(n, me, act):
    def body(d, carry):
        act(lax.rem(me + d, n))
        return carry

    lax.fori_loop(1, n, body, 0)


def enter(n, me):
    barrier = pltpu.get_barrier_semaphore()
    each_peer(n, me, lambda peer: pl.semaphore_signal(
        barrier, inc=1, device_id={"ep": peer}, device_id_type=MESH))
    pl.semaphore_wait(barrier, n - 1)


class Exchange:
    def __init__(self, n, me, source_of, landing, send, recv):
        self.n, self.me, self.source_of = n, me, source_of
        self.landing, self.send, self.recv = landing, send, recv

    def start(self, peer):
        pltpu.make_async_remote_copy(
            src_ref=self.source_of(peer),
            dst_ref=self.landing.at[self.me],
            send_sem=self.send.at[peer],
            recv_sem=self.recv.at[self.me],
            device_id={"ep": peer},
            device_id_type=MESH,
        ).start()

    def start_all(self):
        each_peer(self.n, self.me, self.start)

    def incoming(self, peer):
        return pltpu.make_async_remote_copy(
            src_ref=self.source_of(peer),
            dst_ref=self.landing.at[peer],
            send_sem=self.send.at[peer],
            recv_sem=self.recv.at[peer],
            device_id={"ep": peer},
            device_id_type=MESH,
        )

    def wait_recv(self, then=None):
        def body(d, carry):
            peer = lax.rem(self.me + self.n - d, self.n)
            self.incoming(peer).wait_recv()
            if then is not None:
                then(peer)
            return carry

        lax.fori_loop(1, self.n, body, 0)

    def wait_send(self):
        each_peer(self.n, self.me, lambda peer: self.incoming(peer).wait_send())


class Gather:
    def __init__(self, n, me, source, landing, send, recv, forward):
        self.n, self.me, self.source, self.landing = n, me, source, landing
        self.send, self.recv, self.forward = send, recv, forward
        self.partner = me + 1 - 2 * lax.rem(me, 2)

    def copy(self, source, slot, sem, peer):
        return pltpu.make_async_remote_copy(
            src_ref=source,
            dst_ref=self.landing.at[slot],
            send_sem=sem,
            recv_sem=self.recv.at[slot],
            device_id={"ep": peer},
            device_id_type=MESH,
        )

    def own(self, peer):
        return self.copy(self.source, self.me, self.send.at[peer], peer)

    def onward(self, slot):
        return self.copy(self.landing.at[slot], slot, self.forward.at[slot], self.partner)

    def each(self, act):
        def body(d, carry):
            act(2 * d)
            return carry

        lax.fori_loop(1, self.n // 2, body, 0)

    def start(self):
        self.each(lambda d: self.own(lax.rem(self.me + d, self.n)).start())
        self.own(self.partner).start()

    def arrive(self, slot, then):
        self.copy(self.source, slot, self.send.at[slot], slot).wait_recv()
        then(slot)

    def finish(self, then):
        def pass_on(d):
            slot = lax.rem(self.me + self.n - d, self.n)
            self.copy(self.source, slot, self.send.at[slot], slot).wait_recv()
            self.onward(slot).start()
            then(slot)

        self.each(pass_on)
        self.arrive(self.partner, then)
        self.each(lambda d: self.arrive(lax.rem(self.partner + self.n - d, self.n), then))

    def wait_send(self):
        self.own(self.partner).wait_send()
        self.each(lambda d: self.own(lax.rem(self.me + d, self.n)).wait_send())
        self.each(lambda d: self.onward(lax.rem(self.me + self.n - d, self.n)).wait_send())


def project_kernel(
    n, x_hbm, wr, wk, wv, dli, dlo, dbase_hbm, cri, cro, cbase_hbm,
    rkv_out, decay_out, rate_out,
    weights, dli_v, dlo_v, cri_v, cro_v, x_ref, dbase, cbase, gathered, rows, outs, back,
    local, send1, recv1, send2, recv2, forward,
):
    me = lax.axis_index("ep")
    series, _ = x_ref.shape
    width = wr.shape[1]
    loads = [
        pltpu.make_async_copy(src, dst, local.at[i])
        for i, (src, dst) in enumerate([
            (x_hbm, x_ref), (dli, dli_v), (cri, cri_v), (dlo, dlo_v), (cro, cro_v),
            (dbase_hbm, dbase), (cbase_hbm, cbase),
            (wr, weights.at[0]), (wk, weights.at[1]), (wv, weights.at[2]),
        ])
    ]
    for load in loads:
        load.start()
    enter(n, me)
    loads[0].wait()
    gather = Gather(n, me, x_ref, gathered, send1, recv1, forward)
    gather.start()

    rows[...] = jnp.zeros_like(rows)

    def place(source, block):
        rows[pl.ds(pl.multiple_of(source * PAD, PAD), series), :] = block.astype(F32)

    place(me, x_ref[...])
    own = rows[pl.ds(pl.multiple_of(me * PAD, PAD), PAD), :].astype(BF16)
    for load in loads[1:7]:
        load.wait()
    decay_low = jnp.tanh(contract(own, dli_v[...], (1, 1))).astype(BF16)
    decay_pre = dbase[...] + contract(decay_low, dlo_v[...], (1, 0))
    decay_out[...] = jnp.exp(sigmoid(decay_pre) * -(2.718281828459045**-0.5))
    iclr_low = contract(own, cri_v[...], (1, 1)).astype(BF16)
    rate_out[...] = sigmoid(cbase[...] + contract(iclr_low, cro_v[...], (1, 0)))
    for load in loads[7:]:
        load.wait()

    gather.finish(lambda peer: place(peer, gathered[peer]))
    lhs = rows[...].astype(BF16)
    for c in range(3):
        columns = jnp.dot(lhs, weights[c], preferred_element_type=F32)
        outs[:, c] = columns.reshape(n, PAD, width).astype(BF16)
    spread = Exchange(n, me, lambda peer: outs.at[peer], back, send2, recv2)
    spread.start_all()
    back[me] = outs[me]
    spread.wait_recv()
    for source in range(n):
        for c in range(3):
            rkv_out[c, :, source * width : (source + 1) * width] = back[source, c].astype(F32)
    gather.wait_send()
    spread.wait_send()


def mixer_kernel(
    state, rkv, decay_ref, rate_ref, scale_ref, blend_ref, coef_ref, gain_ref,
    mixed_out, next_hbm, fresh, store_sem,
):
    series, heads, head, _ = state.shape
    per_step = LANES // head
    steps = heads // per_step

    def pair(s):
        return pl.ds(s * per_step, per_step)

    def store(s):
        return pltpu.make_async_copy(
            fresh.at[:, pair(s)], next_hbm.at[:, pair(s)], store_sem.at[s]
        )

    token = lax.broadcasted_iota(jnp.int32, (PAD, head), 0)

    def step(s, carry):
        block = pl.ds(pl.multiple_of(s * LANES, LANES), LANES)
        receptance, key, value = (rkv[c, :, block] for c in range(3))
        decays, rates = decay_ref[:, block], rate_ref[:, block]
        scales, blends, gains = scale_ref[:, block], blend_ref[:, block], gain_ref[:, block]
        pieces = []
        for h in range(per_step):
            part = slice(h * head, (h + 1) * head)
            r, k, v = receptance[:, part], key[:, part], value[:, part]
            decay, rate = decays[:, part], rates[:, part]
            scaled = k * scales[:, part]
            removal = scaled * lax.rsqrt(jnp.sum(scaled * scaled, -1, keepdims=True) + 1e-06)
            key_mod = k * (1.0 + (rate - 1.0) * blends[:, part])
            written = removal * rate
            here = s * per_step + h
            query = decay * r
            def split(values):
                big = values.astype(BF16)
                return big.astype(F32), values - big.astype(F32)

            q_big, q_small = split(query)
            d_big, d_small = split(removal)
            probe = jnp.concatenate([q_big, d_big, q_small, d_small], axis=0).astype(BF16)
            direct = jnp.zeros((PAD, head), F32)
            removed = jnp.zeros((PAD, head), F32)
            for t in range(series):
                old = state[t, here]
                big = old.astype(BF16)
                small = (old - big.astype(F32)).astype(BF16)
                first = contract(probe, big, (1, 1))
                second = contract(probe[: 2 * PAD], small, (1, 1))
                sums = first[: 2 * PAD] + first[2 * PAD :] + second
                direct = jnp.where(token == t, sums[:PAD], direct)
                removed = jnp.where(token == t, sums[PAD:], removed)
            m_big, m_small = split(removed)
            w_big, w_small = split(-written)
            k_big, k_small = split(key_mod)
            left = jnp.concatenate([m_big, m_big, m_small, v, v, jnp.zeros_like(v)], axis=0).astype(BF16)
            for t in range(series):
                only = token == t
                right = jnp.concatenate(
                    [jnp.where(only, x, 0.0) for x in (w_big, w_small, w_big, k_big, k_small)]
                    + [jnp.zeros_like(v)], axis=0
                ).astype(BF16)
                fresh[t, here] = state[t, here] * decay[t : t + 1] + contract(left, right, (0, 0))
            readout = (
                direct
                - removed * jnp.sum(written * r, -1, keepdims=True)
                + v * jnp.sum(key_mod * r, -1, keepdims=True)
            )
            center = jnp.mean(readout, -1, keepdims=True)
            spread = jnp.mean(jnp.square(readout - center), -1, keepdims=True)
            standard = (readout - center) * lax.rsqrt(spread + group_eps) * gains[:, part]
            coef = coef_ref[pl.ds(here, 1), :]
            present = jnp.sum(r * key_mod * coef, -1, keepdims=True) * v
            pieces.append(standard + present)
        mixed_out[:, block] = jnp.concatenate(pieces, axis=1).astype(BF16)
        store(s).start()
        return carry

    lax.fori_loop(0, steps, step, 0)

    def drain(s, carry):
        store(s).wait()
        return carry

    lax.fori_loop(0, steps, drain, 0)


def finish_kernel(
    n, mixed, x_ref, routes, norm_gain, group_router, expert_router, final_gain,
    w_out, w_gate, w_up, w_down,
    tokens_out,
    wo_v, wg_v, wu_v, wd_v, gathered, outs, back, attn, resid, flat, away, arrived, home,
    landed, local, send1, recv1, send2, recv2, send3, recv3, send4, recv4,
    forward,
):
    me = lax.axis_index("ep")
    series, model = x_ref.shape
    width = w_out.shape[1]
    experts = expert_router.shape[0]
    groups = group_router.shape[0]
    top = routes.shape[0]
    loads = [
        pltpu.make_async_copy(src, dst, local.at[i])
        for i, (src, dst) in enumerate(
            [(w_out, wo_v), (w_gate, wg_v), (w_up, wu_v), (w_down, wd_v)]
        )
    ]
    for load in loads:
        load.start()
    enter(n, me)
    gather = Gather(n, me, mixed, gathered, send1, recv1, forward)
    gather.start()
    gathered[me] = mixed[...]
    resid[...] = jnp.zeros_like(resid)
    resid[:series, :] = x_ref[...].astype(F32)

    slots = experts * CAP
    slot_ids = lax.broadcasted_iota(jnp.int32, (slots, PAD), 0)
    named = jnp.zeros((slots, PAD), F32)
    rank = jnp.zeros((slots, PAD), F32)
    for k in range(top):
        offset = slot_ids - routes[k : k + 1, :] * CAP
        match = (offset >= 0) & (offset < CAP)
        named = named + jnp.where(match, 1.0, 0.0)
        rank = rank + jnp.where(match, offset.astype(F32), 0.0)
    earlier = (
        lax.broadcasted_iota(jnp.int32, (PAD, PAD), 0)
        < lax.broadcasted_iota(jnp.int32, (PAD, PAD), 1)
    ).astype(F32)
    before = contract(named, earlier, (1, 0))
    placing = jnp.where(jnp.abs(before - rank) < 0.5, named, 0.0)
    ahead = lax.broadcasted_iota(jnp.int32, (slots, experts), 0) - CAP * (
        lax.broadcasted_iota(jnp.int32, (slots, experts), 1)
    )
    repeat = jnp.where((ahead >= 0) & (ahead < CAP), 1.0, 0.0)

    loads[0].wait()
    gather.finish(lambda peer: None)
    lhs = gathered[...].astype(F32).reshape(n * PAD, model).astype(BF16)
    columns = jnp.dot(lhs, wo_v[...], preferred_element_type=F32)
    outs[...] = columns.reshape(n, PAD, width).astype(BF16)
    spread = Exchange(n, me, lambda peer: outs.at[peer], back, send2, recv2)
    spread.start_all()
    back[me] = outs[me]
    spread.wait_recv()
    for source in range(n):
        attn[:, source * width : (source + 1) * width] = back[source].astype(F32)
    hidden = layer_norm(residual_scale * resid[...] + attn[...], norm_gain[...]).astype(BF16)

    flat[...] = contract(placing.astype(BF16), hidden, (1, 0))

    for e in range(n):
        away[e] = flat[e * CAP : (e + 1) * CAP, :].astype(BF16)
    dispatch = Exchange(n, me, lambda peer: away.at[peer], arrived, send3, recv3)
    dispatch.start_all()
    arrived[me] = away[me]

    group_logits = contract(group_router[...], hidden, (1, 1))
    expert_logits = contract(
        repeat, contract(expert_router[...], hidden, (1, 1)), (1, 0), HIGHEST
    )
    lifted = jnp.exp(group_logits - jnp.max(group_logits, 0, keepdims=True))
    group_ids = lax.broadcasted_iota(jnp.int32, (groups, PAD), 0) * (experts // groups)
    first = routes[0:1, :]
    in_group = (first >= group_ids) & (first < group_ids + experts // groups)
    group_prob = jnp.sum(jnp.where(in_group, lifted, 0.0), 0, keepdims=True) / jnp.sum(
        lifted, 0, keepdims=True
    )
    is_named = named > 0.5
    highest = jnp.max(jnp.where(is_named, expert_logits, -1e30), 0, keepdims=True)
    raised = jnp.where(is_named, jnp.exp(expert_logits - highest), 0.0)
    total = jnp.sum(raised, 0, keepdims=True) / CAP
    gates = group_prob * raised / jnp.where(total > 0.0, total, 1.0)
    weights = gates * placing

    for load in loads[1:]:
        load.wait()

    dispatch.wait_recv()
    for s in range(n):
        flat[s * CAP : (s + 1) * CAP, :] = arrived[s].astype(F32)
    rows = flat[...].astype(BF16)
    gate_part = jnp.dot(rows, wg_v[0], preferred_element_type=F32)
    up_part = jnp.dot(rows, wu_v[0], preferred_element_type=F32)
    act = (gate_part * sigmoid(gate_part) * up_part).astype(BF16)
    flat[...] = jnp.dot(act, wd_v[0], preferred_element_type=F32)

    for s in range(n):
        home[s] = flat[s * CAP : (s + 1) * CAP, :].astype(BF16)
    giveback = Exchange(n, me, lambda peer: home.at[peer], landed, send4, recv4)
    giveback.start_all()
    landed[me] = home[me]

    giveback.wait_recv()
    for e in range(n):
        flat[e * CAP : (e + 1) * CAP, :] = landed[e].astype(F32)
    expert_sum = contract(weights, flat[...], (0, 0), HIGHEST)
    tokens = layer_norm(residual_scale * hidden.astype(F32) + expert_sum, final_gain[...])
    tokens_out[...] = tokens[:series].astype(BF16)
    gather.wait_send()
    spread.wait_send()
    dispatch.wait_send()
    giveback.wait_send()


VMEM = pl.BlockSpec(memory_space=pltpu.VMEM)
ANY = pl.BlockSpec(memory_space=pl.ANY)
HBM = pl.BlockSpec(memory_space=pltpu.HBM)
MIB = 1024 * 1024


def on_device(
    n,
    sequence_input_rows,
    value_key_state,
    receptance_matrix,
    key_matrix,
    value_matrix,
    decay_lowrank_input,
    decay_lowrank_output,
    decay_base_preact,
    context_rate_input,
    context_rate_output,
    context_rate_base,
    removal_key_scale,
    key_context_rate_blend,
    present_item_coefficient,
    head_norm_gain,
    mixer_output_matrix,
    mixer_norm_gain,
    group_router_columns,
    expert_router_columns,
    expert_gate_matrix,
    expert_up_matrix,
    expert_down_matrix,
    final_norm_gain,
    routes,
):
    series, model = sequence_input_rows.shape
    heads, head = present_item_coefficient.shape
    inner = heads * head
    width = receptance_matrix.shape[1]
    out_width = mixer_output_matrix.shape[1]
    experts = expert_router_columns.shape[1]
    low_d, low_a = decay_lowrank_input.shape[1], context_rate_input.shape[1]
    hidden_units = expert_gate_matrix.shape[2]
    assert experts == n

    def row(values):
        return values.reshape(1, -1)

    dma = pltpu.SemaphoreType.DMA
    rkv, decay, rate = pl.pallas_call(
        functools.partial(project_kernel, n),
        out_shape=[
            jax.ShapeDtypeStruct((3, PAD, inner), F32),
            jax.ShapeDtypeStruct((PAD, inner), F32),
            jax.ShapeDtypeStruct((PAD, inner), F32),
        ],
        in_specs=[HBM] * 10,
        out_specs=[VMEM] * 3,
        scratch_shapes=[
            pltpu.VMEM((3, model, width), BF16),
            pltpu.VMEM((low_d, model), BF16),
            pltpu.VMEM((low_d, inner), BF16),
            pltpu.VMEM((low_a, model), BF16),
            pltpu.VMEM((low_a, inner), BF16),
            pltpu.VMEM((series, model), BF16),
            pltpu.VMEM((1, inner), F32),
            pltpu.VMEM((1, inner), F32),
            pltpu.VMEM((n, series, model), BF16),
            pltpu.VMEM((n * PAD, model), F32),
            pltpu.VMEM((n, 3, PAD, width), BF16),
            pltpu.VMEM((n, 3, PAD, width), BF16),
            dma((10,)),
        ]
        + [dma((n,))] * 5,
        compiler_params=pltpu.CompilerParams(
            collective_id=0, has_side_effects=True, vmem_limit_bytes=24 * MIB
        ),
        cost_estimate=pl.CostEstimate(flops=20_000_000_000, bytes_accessed=40_000_000, transcendentals=0),
        name="project",
    )(
        *(
            pltpu.with_memory_space_constraint(operand, pltpu.HBM)
            for operand in (
                sequence_input_rows,
                receptance_matrix,
                key_matrix,
                value_matrix,
                decay_lowrank_input.T,
                decay_lowrank_output,
                row(decay_base_preact),
                context_rate_input.T,
                context_rate_output,
                row(context_rate_base),
            )
        )
    )

    steps = heads // (LANES // head)
    mixed, next_recurrent_state = pl.pallas_call(
        mixer_kernel,
        out_shape=[
            jax.ShapeDtypeStruct((PAD, inner), BF16),
            jax.ShapeDtypeStruct(value_key_state.shape, F32),
        ],
        in_specs=[VMEM] * 8,
        out_specs=[VMEM, HBM],
        scratch_shapes=[pltpu.VMEM(value_key_state.shape, F32), dma((steps,))],
        compiler_params=pltpu.CompilerParams(vmem_limit_bytes=24 * MIB),
        name="mixer",
    )(
        value_key_state,
        rkv,
        decay,
        rate,
        row(removal_key_scale),
        row(key_context_rate_blend),
        present_item_coefficient,
        row(head_norm_gain),
    )

    routes_t = jnp.pad(routes.T, ((0, 0), (0, PAD - series)), constant_values=-1)
    tokens_out = pl.pallas_call(
        functools.partial(finish_kernel, n),
        out_shape=jax.ShapeDtypeStruct((series, model), BF16),
        in_specs=[VMEM] * 7 + [ANY] * 4,
        out_specs=VMEM,
        scratch_shapes=[
            pltpu.VMEM((inner, out_width), BF16),
            pltpu.VMEM((1, model, hidden_units), BF16),
            pltpu.VMEM((1, model, hidden_units), BF16),
            pltpu.VMEM((1, hidden_units, model), BF16),
            pltpu.VMEM((n, PAD, inner), BF16),
            pltpu.VMEM((n, PAD, out_width), BF16),
            pltpu.VMEM((n, PAD, out_width), BF16),
            pltpu.VMEM((PAD, model), F32),
            pltpu.VMEM((PAD, model), F32),
            pltpu.VMEM((experts * CAP, model), F32),
        ]
        + [pltpu.VMEM((n, CAP, model), BF16)] * 4
        + [dma((4,))]
        + [dma((n,))] * 9,
        compiler_params=pltpu.CompilerParams(
            collective_id=1, has_side_effects=True, vmem_limit_bytes=24 * MIB
        ),
        cost_estimate=pl.CostEstimate(flops=20_000_000_000, bytes_accessed=40_000_000, transcendentals=0),
        name="finish",
    )(
        mixed,
        sequence_input_rows,
        routes_t,
        row(mixer_norm_gain),
        group_router_columns.T,
        expert_router_columns.T,
        row(final_norm_gain),
        mixer_output_matrix,
        expert_gate_matrix,
        expert_up_matrix,
        expert_down_matrix,
    )
    return (tokens_out, next_recurrent_state)


def solution(mesh):
    in_specs = (
        P(("grp", "ep"), None),
        P(("grp", "ep"), None, None, None),
        P(None, "ep"),
        P(None, "ep"),
        P(None, "ep"),
        P(),
        P(),
        P(),
        P(),
        P(),
        P(),
        P(),
        P(),
        P(),
        P(),
        P(None, "ep"),
        P(),
        P(),
        P(),
        P("ep", None, None),
        P("ep", None, None),
        P("ep", None, None),
        P(),
        P(("grp", "ep"), None),
    )
    out_specs = (P(("grp", "ep"), None), P(("grp", "ep"), None, None, None))
    return jax.shard_map(
        functools.partial(on_device, mesh.shape["ep"]),
        mesh=mesh, in_specs=in_specs, out_specs=out_specs, check_vma=False,
    )
```

```python
import functools

import jax
import jax.numpy as jnp
from jax import lax
from jax.experimental import pallas as pl
from jax.experimental.pallas import tpu as pltpu
from jax.sharding import PartitionSpec as P

CAP = 2
PAD = 8
LANES = 128

residual_scale = 8.0**0.25
norm_eps = 1e-05
group_eps = 0.00064

MESH = pl.DeviceIdType.MESH
F32 = jnp.float32
BF16 = jnp.bfloat16
HIGHEST = lax.Precision.HIGHEST


def layer_norm(values, norm_gain):
    center = jnp.mean(values, -1, keepdims=True)
    spread = jnp.mean(jnp.square(values - center), -1, keepdims=True)
    return (values - center) * lax.rsqrt(spread + norm_eps) * norm_gain


def contract(a, b, dims, precision=None):
    return lax.dot_general(a, b, ((dims[:1], dims[1:]), ((), ())), precision=precision,
                           preferred_element_type=F32)


def sigmoid(values):
    return 1.0 / (1.0 + jnp.exp(-values))


def each_peer(n, me, act):
    def body(d, carry):
        act(lax.rem(me + d, n))
        return carry

    lax.fori_loop(1, n, body, 0)


def enter(n, me):
    barrier = pltpu.get_barrier_semaphore()
    each_peer(n, me, lambda peer: pl.semaphore_signal(
        barrier, inc=1, device_id={"ep": peer}, device_id_type=MESH))
    pl.semaphore_wait(barrier, n - 1)


class Exchange:
    def __init__(self, n, me, source_of, landing, send, recv):
        self.n, self.me, self.source_of = n, me, source_of
        self.landing, self.send, self.recv = landing, send, recv

    def start(self, peer):
        pltpu.make_async_remote_copy(
            src_ref=self.source_of(peer),
            dst_ref=self.landing.at[self.me],
            send_sem=self.send.at[peer],
            recv_sem=self.recv.at[self.me],
            device_id={"ep": peer},
            device_id_type=MESH,
        ).start()

    def start_all(self):
        each_peer(self.n, self.me, self.start)

    def incoming(self, peer):
        return pltpu.make_async_remote_copy(
            src_ref=self.source_of(peer),
            dst_ref=self.landing.at[peer],
            send_sem=self.send.at[peer],
            recv_sem=self.recv.at[peer],
            device_id={"ep": peer},
            device_id_type=MESH,
        )

    def wait_recv(self, then=None):
        def body(d, carry):
            peer = lax.rem(self.me + self.n - d, self.n)
            self.incoming(peer).wait_recv()
            if then is not None:
                then(peer)
            return carry

        lax.fori_loop(1, self.n, body, 0)

    def wait_send(self):
        each_peer(self.n, self.me, lambda peer: self.incoming(peer).wait_send())


class Gather:
    def __init__(self, n, me, source, landing, send, recv, forward):
        self.n, self.me, self.source, self.landing = n, me, source, landing
        self.send, self.recv, self.forward = send, recv, forward
        self.partner = me + 1 - 2 * lax.rem(me, 2)

    def copy(self, source, slot, sem, peer):
        return pltpu.make_async_remote_copy(
            src_ref=source,
            dst_ref=self.landing.at[slot],
            send_sem=sem,
            recv_sem=self.recv.at[slot],
            device_id={"ep": peer},
            device_id_type=MESH,
        )

    def own(self, peer):
        return self.copy(self.source, self.me, self.send.at[peer], peer)

    def onward(self, slot):
        return self.copy(self.landing.at[slot], slot, self.forward.at[slot], self.partner)

    def each(self, act):
        def body(d, carry):
            act(2 * d)
            return carry

        lax.fori_loop(1, self.n // 2, body, 0)

    def start(self):
        self.each(lambda d: self.own(lax.rem(self.me + d, self.n)).start())
        self.own(self.partner).start()

    def arrive(self, slot, then):
        self.copy(self.source, slot, self.send.at[slot], slot).wait_recv()
        then(slot)

    def finish(self, then):
        def pass_on(d):
            slot = lax.rem(self.me + self.n - d, self.n)
            self.copy(self.source, slot, self.send.at[slot], slot).wait_recv()
            self.onward(slot).start()
            then(slot)

        self.each(pass_on)
        self.arrive(self.partner, then)
        self.each(lambda d: self.arrive(lax.rem(self.partner + self.n - d, self.n), then))

    def wait_send(self):
        self.own(self.partner).wait_send()
        self.each(lambda d: self.own(lax.rem(self.me + d, self.n)).wait_send())
        self.each(lambda d: self.onward(lax.rem(self.me + self.n - d, self.n)).wait_send())


def project_kernel(
    n, x_hbm, wr, wk, wv, dli, dlo, dbase_hbm, cri, cro, cbase_hbm,
    rkv_out, decay_out, rate_out,
    weights, dli_v, dlo_v, cri_v, cro_v, x_ref, dbase, cbase, gathered, rows, outs, back,
    local, send1, recv1, send2, recv2, forward,
):
    me = lax.axis_index("ep")
    series, _ = x_ref.shape
    width = wr.shape[1]
    loads = [
        pltpu.make_async_copy(src, dst, local.at[i])
        for i, (src, dst) in enumerate([
            (x_hbm, x_ref), (dli, dli_v), (cri, cri_v), (dlo, dlo_v), (cro, cro_v),
            (dbase_hbm, dbase), (cbase_hbm, cbase),
            (wr, weights.at[0]), (wk, weights.at[1]), (wv, weights.at[2]),
        ])
    ]
    for load in loads:
        load.start()
    enter(n, me)
    loads[0].wait()
    gather = Gather(n, me, x_ref, gathered, send1, recv1, forward)
    gather.start()

    rows[...] = jnp.zeros_like(rows)

    def place(source, block):
        rows[pl.ds(pl.multiple_of(source * PAD, PAD), series), :] = block.astype(F32)

    place(me, x_ref[...])
    own = rows[pl.ds(pl.multiple_of(me * PAD, PAD), PAD), :].astype(BF16)
    for load in loads[1:7]:
        load.wait()
    decay_low = jnp.tanh(contract(own, dli_v[...], (1, 1))).astype(BF16)
    decay_pre = dbase[...] + contract(decay_low, dlo_v[...], (1, 0))
    decay_out[...] = jnp.exp(sigmoid(decay_pre) * -(2.718281828459045**-0.5))
    iclr_low = contract(own, cri_v[...], (1, 1)).astype(BF16)
    rate_out[...] = sigmoid(cbase[...] + contract(iclr_low, cro_v[...], (1, 0)))
    for load in loads[7:]:
        load.wait()

    gather.finish(lambda peer: place(peer, gathered[peer]))
    lhs = rows[...].astype(BF16)
    for c in range(3):
        columns = jnp.dot(lhs, weights[c], preferred_element_type=F32)
        outs[:, c] = columns.reshape(n, PAD, width).astype(BF16)
    spread = Exchange(n, me, lambda peer: outs.at[peer], back, send2, recv2)
    spread.start_all()
    back[me] = outs[me]
    spread.wait_recv()
    for source in range(n):
        for c in range(3):
            rkv_out[c, :, source * width : (source + 1) * width] = back[source, c].astype(F32)
    gather.wait_send()
    spread.wait_send()


def mixer_kernel(
    state, rkv, decay_ref, rate_ref, scale_ref, blend_ref, coef_ref, gain_ref,
    mixed_out, next_hbm, fresh, store_sem,
):
    series, heads, head, _ = state.shape
    steps, = store_sem.shape
    per_step = heads // steps
    span = per_step * head
    mine = range(per_step)

    def store(s):
        group = pl.ds(s * per_step, per_step)
        return pltpu.make_async_copy(
            fresh.at[:, group], next_hbm.at[:, group], store_sem.at[s]
        )

    token = lax.broadcasted_iota(jnp.int32, (PAD, head), 0)

    def split(values):
        big = values.astype(BF16)
        return big.astype(F32), values - big.astype(F32)

    def total(values):
        return jnp.sum(values, -1, keepdims=True)

    def step(s, carry):
        block = pl.ds(pl.multiple_of(s * span, LANES), span)

        def per_head(values):
            return [values[:, h * head : (h + 1) * head] for h in mine]

        r, k, v = (per_head(rkv[c, :, block]) for c in range(3))
        decay, rate = per_head(decay_ref[:, block]), per_head(rate_ref[:, block])
        scale, blend = per_head(scale_ref[:, block]), per_head(blend_ref[:, block])
        gain = per_head(gain_ref[:, block])
        scaled = [k[h] * scale[h] for h in mine]
        norms = [total(scaled[h] * scaled[h]) for h in mine]
        removal = [scaled[h] * lax.rsqrt(norms[h] + 1e-06) for h in mine]
        key_mod = [k[h] * (1.0 + (rate[h] - 1.0) * blend[h]) for h in mine]
        written = [removal[h] * rate[h] for h in mine]
        coef = [coef_ref[pl.ds(s * per_step + h, 1), :] for h in mine]
        gone_along = [total(written[h] * r[h]) for h in mine]
        new_along = [total(key_mod[h] * r[h]) for h in mine]
        present = [total(r[h] * key_mod[h] * coef[h]) * v[h] for h in mine]
        probe = []
        for h in mine:
            q_big, q_small = split(decay[h] * r[h])
            d_big, d_small = split(removal[h])
            probe.append(
                jnp.concatenate([q_big, d_big, q_small, d_small], axis=0).astype(BF16)
            )
        direct = [jnp.zeros((PAD, head), F32) for h in mine]
        removed = [jnp.zeros((PAD, head), F32) for h in mine]
        for t in range(series):
            for h in mine:
                old = state[t, s * per_step + h]
                big = old.astype(BF16)
                small = (old - big.astype(F32)).astype(BF16)
                first = contract(probe[h], big, (1, 1))
                second = contract(probe[h][: 2 * PAD], small, (1, 1))
                sums = first[: 2 * PAD] + first[2 * PAD :] + second
                direct[h] = jnp.where(token == t, sums[:PAD], direct[h])
                removed[h] = jnp.where(token == t, sums[PAD:], removed[h])
        left, terms = [], []
        for h in mine:
            m_big, m_small = split(removed[h])
            w_big, w_small = split(-written[h])
            k_big, k_small = split(key_mod[h])
            nothing = jnp.zeros_like(v[h])
            left.append(
                jnp.concatenate(
                    [m_big, m_big, m_small, v[h], v[h], nothing], axis=0
                ).astype(BF16)
            )
            terms.append((w_big, w_small, w_big, k_big, k_small, nothing))
        for t in range(series):
            for h in mine:
                right = jnp.concatenate(
                    [jnp.where(token == t, x, 0.0) for x in terms[h]], axis=0
                ).astype(BF16)
                here = s * per_step + h
                fresh[t, here] = state[t, here] * decay[h][t : t + 1] + contract(
                    left[h], right, (0, 0)
                )
        store(s).start()
        readout = [
            direct[h] - removed[h] * gone_along[h] + v[h] * new_along[h] for h in mine
        ]
        center = [total(readout[h]) * (1.0 / head) for h in mine]
        spread = [total(jnp.square(readout[h] - center[h])) * (1.0 / head) for h in mine]
        pieces = [
            (readout[h] - center[h]) * lax.rsqrt(spread[h] + group_eps) * gain[h] + present[h]
            for h in mine
        ]
        mixed_out[:, block] = jnp.concatenate(pieces, axis=1).astype(BF16)
        return carry

    lax.fori_loop(0, steps, step, 0)

    def drain(s, carry):
        store(s).wait()
        return carry

    lax.fori_loop(0, steps, drain, 0)


def finish_kernel(
    n, mixed, x_ref, routes, norm_gain, group_router, expert_router, final_gain,
    w_out, w_gate, w_up, w_down,
    tokens_out,
    wo_v, wg_v, wu_v, wd_v, gathered, outs, back, attn, resid, flat, away, arrived, home,
    landed, local, send1, recv1, send2, recv2, send3, recv3, send4, recv4,
    forward,
):
    me = lax.axis_index("ep")
    series, model = x_ref.shape
    width = w_out.shape[1]
    experts = expert_router.shape[0]
    groups = group_router.shape[0]
    top = routes.shape[0]
    loads = [
        pltpu.make_async_copy(src, dst, local.at[i])
        for i, (src, dst) in enumerate(
            [(w_out, wo_v), (w_gate, wg_v), (w_up, wu_v), (w_down, wd_v)]
        )
    ]
    for load in loads:
        load.start()
    enter(n, me)
    gather = Gather(n, me, mixed, gathered, send1, recv1, forward)
    gather.start()
    gathered[me] = mixed[...]
    resid[...] = jnp.zeros_like(resid)
    resid[:series, :] = x_ref[...].astype(F32)

    slots = experts * CAP
    slot_ids = lax.broadcasted_iota(jnp.int32, (slots, PAD), 0)
    named = jnp.zeros((slots, PAD), F32)
    rank = jnp.zeros((slots, PAD), F32)
    for k in range(top):
        offset = slot_ids - routes[k : k + 1, :] * CAP
        match = (offset >= 0) & (offset < CAP)
        named = named + jnp.where(match, 1.0, 0.0)
        rank = rank + jnp.where(match, offset.astype(F32), 0.0)
    earlier = (
        lax.broadcasted_iota(jnp.int32, (PAD, PAD), 0)
        < lax.broadcasted_iota(jnp.int32, (PAD, PAD), 1)
    ).astype(F32)
    before = contract(named, earlier, (1, 0))
    placing = jnp.where(jnp.abs(before - rank) < 0.5, named, 0.0)
    ahead = lax.broadcasted_iota(jnp.int32, (slots, experts), 0) - CAP * (
        lax.broadcasted_iota(jnp.int32, (slots, experts), 1)
    )
    repeat = jnp.where((ahead >= 0) & (ahead < CAP), 1.0, 0.0)

    loads[0].wait()
    gather.finish(lambda peer: None)
    lhs = gathered[...].astype(F32).reshape(n * PAD, model).astype(BF16)
    columns = jnp.dot(lhs, wo_v[...], preferred_element_type=F32)
    outs[...] = columns.reshape(n, PAD, width).astype(BF16)
    spread = Exchange(n, me, lambda peer: outs.at[peer], back, send2, recv2)
    spread.start_all()
    back[me] = outs[me]
    spread.wait_recv()
    for source in range(n):
        attn[:, source * width : (source + 1) * width] = back[source].astype(F32)
    hidden = layer_norm(residual_scale * resid[...] + attn[...], norm_gain[...]).astype(BF16)

    flat[...] = contract(placing.astype(BF16), hidden, (1, 0))

    for e in range(n):
        away[e] = flat[e * CAP : (e + 1) * CAP, :].astype(BF16)
    dispatch = Exchange(n, me, lambda peer: away.at[peer], arrived, send3, recv3)
    dispatch.start_all()
    arrived[me] = away[me]

    group_logits = contract(group_router[...], hidden, (1, 1))
    expert_logits = contract(
        repeat, contract(expert_router[...], hidden, (1, 1)), (1, 0), HIGHEST
    )
    lifted = jnp.exp(group_logits - jnp.max(group_logits, 0, keepdims=True))
    group_ids = lax.broadcasted_iota(jnp.int32, (groups, PAD), 0) * (experts // groups)
    first = routes[0:1, :]
    in_group = (first >= group_ids) & (first < group_ids + experts // groups)
    group_prob = jnp.sum(jnp.where(in_group, lifted, 0.0), 0, keepdims=True) / jnp.sum(
        lifted, 0, keepdims=True
    )
    is_named = named > 0.5
    highest = jnp.max(jnp.where(is_named, expert_logits, -1e30), 0, keepdims=True)
    raised = jnp.where(is_named, jnp.exp(expert_logits - highest), 0.0)
    total = jnp.sum(raised, 0, keepdims=True) / CAP
    gates = group_prob * raised / jnp.where(total > 0.0, total, 1.0)
    weights = gates * placing

    for load in loads[1:]:
        load.wait()

    dispatch.wait_recv()
    for s in range(n):
        flat[s * CAP : (s + 1) * CAP, :] = arrived[s].astype(F32)
    rows = flat[...].astype(BF16)
    gate_part = jnp.dot(rows, wg_v[0], preferred_element_type=F32)
    up_part = jnp.dot(rows, wu_v[0], preferred_element_type=F32)
    act = (gate_part * sigmoid(gate_part) * up_part).astype(BF16)
    flat[...] = jnp.dot(act, wd_v[0], preferred_element_type=F32)

    for s in range(n):
        home[s] = flat[s * CAP : (s + 1) * CAP, :].astype(BF16)
    giveback = Exchange(n, me, lambda peer: home.at[peer], landed, send4, recv4)
    giveback.start_all()
    landed[me] = home[me]

    giveback.wait_recv()
    for e in range(n):
        flat[e * CAP : (e + 1) * CAP, :] = landed[e].astype(F32)
    expert_sum = contract(weights, flat[...], (0, 0), HIGHEST)
    tokens = layer_norm(residual_scale * hidden.astype(F32) + expert_sum, final_gain[...])
    tokens_out[...] = tokens[:series].astype(BF16)
    gather.wait_send()
    spread.wait_send()
    dispatch.wait_send()
    giveback.wait_send()


VMEM = pl.BlockSpec(memory_space=pltpu.VMEM)
ANY = pl.BlockSpec(memory_space=pl.ANY)
HBM = pl.BlockSpec(memory_space=pltpu.HBM)
MIB = 1024 * 1024


def on_device(
    n,
    sequence_input_rows,
    value_key_state,
    receptance_matrix,
    key_matrix,
    value_matrix,
    decay_lowrank_input,
    decay_lowrank_output,
    decay_base_preact,
    context_rate_input,
    context_rate_output,
    context_rate_base,
    removal_key_scale,
    key_context_rate_blend,
    present_item_coefficient,
    head_norm_gain,
    mixer_output_matrix,
    mixer_norm_gain,
    group_router_columns,
    expert_router_columns,
    expert_gate_matrix,
    expert_up_matrix,
    expert_down_matrix,
    final_norm_gain,
    routes,
):
    series, model = sequence_input_rows.shape
    heads, head = present_item_coefficient.shape
    inner = heads * head
    width = receptance_matrix.shape[1]
    out_width = mixer_output_matrix.shape[1]
    experts = expert_router_columns.shape[1]
    low_d, low_a = decay_lowrank_input.shape[1], context_rate_input.shape[1]
    hidden_units = expert_gate_matrix.shape[2]
    assert experts == n

    def row(values):
        return values.reshape(1, -1)

    dma = pltpu.SemaphoreType.DMA
    rkv, decay, rate = pl.pallas_call(
        functools.partial(project_kernel, n),
        out_shape=[
            jax.ShapeDtypeStruct((3, PAD, inner), F32),
            jax.ShapeDtypeStruct((PAD, inner), F32),
            jax.ShapeDtypeStruct((PAD, inner), F32),
        ],
        in_specs=[HBM] * 10,
        out_specs=[VMEM] * 3,
        scratch_shapes=[
            pltpu.VMEM((3, model, width), BF16),
            pltpu.VMEM((low_d, model), BF16),
            pltpu.VMEM((low_d, inner), BF16),
            pltpu.VMEM((low_a, model), BF16),
            pltpu.VMEM((low_a, inner), BF16),
            pltpu.VMEM((series, model), BF16),
            pltpu.VMEM((1, inner), F32),
            pltpu.VMEM((1, inner), F32),
            pltpu.VMEM((n, series, model), BF16),
            pltpu.VMEM((n * PAD, model), F32),
            pltpu.VMEM((n, 3, PAD, width), BF16),
            pltpu.VMEM((n, 3, PAD, width), BF16),
            dma((10,)),
        ]
        + [dma((n,))] * 5,
        compiler_params=pltpu.CompilerParams(
            collective_id=0, has_side_effects=True, vmem_limit_bytes=24 * MIB
        ),
        cost_estimate=pl.CostEstimate(flops=20_000_000_000, bytes_accessed=40_000_000, transcendentals=0),
        name="project",
    )(
        *(
            pltpu.with_memory_space_constraint(operand, pltpu.HBM)
            for operand in (
                sequence_input_rows,
                receptance_matrix,
                key_matrix,
                value_matrix,
                decay_lowrank_input.T,
                decay_lowrank_output,
                row(decay_base_preact),
                context_rate_input.T,
                context_rate_output,
                row(context_rate_base),
            )
        )
    )

    steps = heads // (2 * LANES // head)
    mixed, next_recurrent_state = pl.pallas_call(
        mixer_kernel,
        out_shape=[
            jax.ShapeDtypeStruct((PAD, inner), BF16),
            jax.ShapeDtypeStruct(value_key_state.shape, F32),
        ],
        in_specs=[VMEM] * 8,
        out_specs=[VMEM, HBM],
        scratch_shapes=[pltpu.VMEM(value_key_state.shape, F32), dma((steps,))],
        compiler_params=pltpu.CompilerParams(vmem_limit_bytes=24 * MIB),
        name="mixer",
    )(
        value_key_state,
        rkv,
        decay,
        rate,
        row(removal_key_scale),
        row(key_context_rate_blend),
        present_item_coefficient,
        row(head_norm_gain),
    )

    routes_t = jnp.pad(routes.T, ((0, 0), (0, PAD - series)), constant_values=-1)
    tokens_out = pl.pallas_call(
        functools.partial(finish_kernel, n),
        out_shape=jax.ShapeDtypeStruct((series, model), BF16),
        in_specs=[VMEM] * 7 + [ANY] * 4,
        out_specs=VMEM,
        scratch_shapes=[
            pltpu.VMEM((inner, out_width), BF16),
            pltpu.VMEM((1, model, hidden_units), BF16),
            pltpu.VMEM((1, model, hidden_units), BF16),
            pltpu.VMEM((1, hidden_units, model), BF16),
            pltpu.VMEM((n, PAD, inner), BF16),
            pltpu.VMEM((n, PAD, out_width), BF16),
            pltpu.VMEM((n, PAD, out_width), BF16),
            pltpu.VMEM((PAD, model), F32),
            pltpu.VMEM((PAD, model), F32),
            pltpu.VMEM((experts * CAP, model), F32),
        ]
        + [pltpu.VMEM((n, CAP, model), BF16)] * 4
        + [dma((4,))]
        + [dma((n,))] * 9,
        compiler_params=pltpu.CompilerParams(
            collective_id=1, has_side_effects=True, vmem_limit_bytes=24 * MIB
        ),
        cost_estimate=pl.CostEstimate(flops=20_000_000_000, bytes_accessed=40_000_000, transcendentals=0),
        name="finish",
    )(
        mixed,
        sequence_input_rows,
        routes_t,
        row(mixer_norm_gain),
        group_router_columns.T,
        expert_router_columns.T,
        row(final_norm_gain),
        mixer_output_matrix,
        expert_gate_matrix,
        expert_up_matrix,
        expert_down_matrix,
    )
    return (tokens_out, next_recurrent_state)


def solution(mesh):
    in_specs = (
        P(("grp", "ep"), None),
        P(("grp", "ep"), None, None, None),
        P(None, "ep"),
        P(None, "ep"),
        P(None, "ep"),
        P(),
        P(),
        P(),
        P(),
        P(),
        P(),
        P(),
        P(),
        P(),
        P(),
        P(None, "ep"),
        P(),
        P(),
        P(),
        P("ep", None, None),
        P("ep", None, None),
        P("ep", None, None),
        P(),
        P(("grp", "ep"), None),
    )
    out_specs = (P(("grp", "ep"), None), P(("grp", "ep"), None, None, None))
    return jax.shard_map(
        functools.partial(on_device, mesh.shape["ep"]),
        mesh=mesh, in_specs=in_specs, out_specs=out_specs, check_vma=False,
    )
```
